32 devices in a mesh: ep: 8 (over z, x), tp: 4 (over y, core).
Axes of the slice: x: 2, y: 2, z: 4, core: 2. Of those that a mesh axis runs over, the one named last changes fastest.
Arguments:
- tokens: bfloat16 [2048, 2048], P('ep'), may hold values from -6 to 6
- routes: int32 [2048, 2], P('ep'), may hold values from 0 to 7, all different within a row; in each aligned block of 256 rows (0 to 255, 256 to 511, ...) at most 128 rows name the same one
- router_matrix: bfloat16 [2048, 8], replicated, may hold values from -0.125 to 0.125
- cotangent: bfloat16 [2048, 2048], P('ep', 'tp'), may hold values from -3 to 3
- gate_proj: bfloat16 [8, 2048, 3584], P('ep', None, 'tp'), may hold values from -0.125 to 0.125
- up_proj: bfloat16 [8, 2048, 3584], P('ep', None, 'tp'), may hold values from -0.125 to 0.125
- down_proj: bfloat16 [8, 3584, 2048], P('ep', 'tp'), may hold values from -0.09375 to 0.09375
Outputs:
- token_grad: bfloat16 [2048, 2048], P('ep', 'tp')
- mixing_grad: float32 [2048, 2], P('ep')
- router_grad: float32 [2048, 8], P(('ep', 'tp'))
- gate_grad: bfloat16 [8, 2048, 3584], P('ep', None, 'tp')
- up_grad: bfloat16 [8, 2048, 3584], P('ep', None, 'tp')
- down_grad: bfloat16 [8, 3584, 2048], P('ep', 'tp')
The draws below stay inside these ranges and needn't reach their ends.
Inputs may be any that keep to these rules, and one draw needn't show every extreme that they name: `routes`: the two experts of a row differ. In each aligned block of 256 rows no expert is named by more than 128 rows, a bound that some block reaches; every expert is named somewhere.
All inputs are finite; a program needn't handle non-finite values.
Results may differ from the reference program's by a relative error of at most 0.019.
Values may be sent and summed in bfloat16 or wider, within the bound.
A program may use at most 128 MiB of HBM per device.

```python
import math
import jax
import jax.numpy as jnp
import numpy as np
from jax import lax

D = 2048
FF = 3584
TOP = 2
TOK_DEV = 256
EXPERTS = 8
TOKENS = 2048
CAP = 128
N_EP = 8
N_TP = 4


def steps_of(rng, extent, cuts, least, top_value):
    gain = 1.0
    for dim, shards_of in cuts:
        draws = jax.random.uniform(jax.random.fold_in(jax.random.fold_in(rng, 6), dim), (shards_of,), jnp.float32, least / len(cuts), top_value / len(cuts))
        gain = gain * jnp.repeat(jnp.exp(draws), extent[dim] // shards_of).reshape((-1,) + (1,) * (len(extent) - 1 - dim))
    return gain


def routed_block(own_key, own, number, rows, amount, top, most, slope):
    ranking = jax.random.permutation(own_key, amount)
    heavy_load, common = portions_of(amount, rows * top, most, slope, True), portions_of(amount, rows * top, most, slope, False)
    places = jnp.arange(amount)

    def named(tallies, rotation):
        used = int((tallies > 0).sum())
        fixed = max(1, used // 4)
        shifted = fixed + (places - fixed + rotation * (used - fixed)) % max(1, amount - fixed)
        return jnp.zeros((amount,), jnp.int32).at[ranking[jnp.where(places < fixed, places, shifted)]].set(jnp.asarray(tallies, jnp.int32))

    tallies = jnp.where(number % 4 == 0, named(heavy_load, number // 4), named(common, number - number // 4 - 1))
    mixed = jax.random.permutation(jax.random.fold_in(own, 3), amount)
    donor, sink = mixed[0:amount // 2 * 2:2], mixed[1:amount // 2 * 2:2]
    slack = jnp.minimum(tallies[donor] - 1, most - tallies[sink]) // 2
    slack = jnp.where((donor == ranking[0]) | (sink == ranking[0]) | (tallies[sink] == 0), 0, jnp.maximum(slack, 0))
    shifted = jax.random.randint(jax.random.fold_in(own, 4), (amount // 2,), 0, 1 << 20) % (slack + 1)
    tallies = tallies.at[donor].add(-shifted).at[sink].add(shifted)
    items = jnp.searchsorted(jnp.cumsum(tallies), jnp.arange(rows * top), side="right").astype(jnp.int32)
    table = items.reshape(top, rows).T
    table = table[jax.random.permutation(jax.random.fold_in(own, 1), rows)]
    rotation = jax.random.randint(jax.random.fold_in(own, 2), (rows, 1), 0, top)
    return jnp.take_along_axis(table, (jnp.arange(top)[None, :] + rotation) % top, axis=1)


def portions_of(number_of, total, limit, slope, full):
    weights = [(1 << 20) // math.isqrt(standing ** slope) + 1 for standing in range(1, number_of + 1)]
    largest = limit if full else min(limit, max(-(-total // number_of), total * weights[0] // sum(weights)))
    least = 1 if total - largest >= number_of - 1 else 0
    holding, surplus = [largest] + [least] * (number_of - 1), total - largest - least * (number_of - 1)
    while surplus > 0:
        movable = [i for i in range(1, number_of) if holding[i] < largest] or [i for i in range(1, number_of) if holding[i] < limit]
        whole, budget = sum([weights[i] for i in movable]), surplus
        for i in movable:
            addition = min(limit - holding[i], max(1, budget * weights[i] // whole), surplus)
            holding[i] = holding[i] + addition
            surplus = surplus - addition
    return np.array(holding)


def normal_values(own_key, dims, deviation, bound, split=(), kind=jnp.bfloat16):
    drawn = deviation * jax.random.normal(own_key, dims, jnp.float32)
    if split:
        drawn = drawn * steps_of(own_key, dims, split, -0.22, 0.18)
    return jnp.clip(drawn, -bound, bound).astype(kind)


def setup_inputs(seed: int = 0) -> dict:
    key_of = jax.random.split(jax.random.key(seed), 8)
    tokens = normal_values(key_of[0], (TOKENS, D), 1.0, 6.0, ((0, 8),))
    routes_keys = jax.random.split(jax.random.fold_in(key_of[1], 1), TOKENS // TOK_DEV)
    routes_turns = jax.random.permutation(jax.random.fold_in(key_of[1], 3), TOKENS // TOK_DEV)
    routes = jax.vmap(lambda own, number: routed_block(jax.random.fold_in(key_of[1], 2), own, number, TOK_DEV, EXPERTS, TOP, CAP, 2))(routes_keys, routes_turns).reshape((TOKENS, TOP))
    router_matrix = normal_values(key_of[2], (D, EXPERTS), D ** -0.5, 0.125)
    cotangent = normal_values(key_of[3], (TOKENS, D), 0.5, 3.0, ((0, 8), (1, 4)))
    gate_proj = normal_values(key_of[4], (EXPERTS, D, FF), D ** -0.5, 0.125, ((0, 8), (2, 4)))
    up_proj = normal_values(key_of[5], (EXPERTS, D, FF), D ** -0.5, 0.125, ((0, 8), (2, 4)))
    down_proj = normal_values(key_of[6], (EXPERTS, FF, D), FF ** -0.5, 0.09375, ((0, 8), (1, 4)))
    return {"tokens": tokens, "routes": routes, "router_matrix": router_matrix, "cotangent": cotangent, "gate_proj": gate_proj, "up_proj": up_proj, "down_proj": down_proj}


def slot_places(flat_routes, experts, capacity):
    onehot = (flat_routes[:, None] == jnp.arange(experts, dtype=jnp.int32)[None, :]).astype(jnp.int32)
    earlier = jnp.cumsum(onehot, axis=0) - onehot
    places = (flat_routes * capacity + lax.optimization_barrier(jnp.sum(earlier * onehot, axis=1))).astype(jnp.int32)
    entries = flat_routes.shape[0]
    filler = jnp.full((experts * capacity,), entries, jnp.int32).at[places].set(jnp.arange(entries, dtype=jnp.int32))
    return (places, filler)

def expert_pass(operands):
    token_rows, output_rows, mix_rows, w_gate, w_up, w_down = operands
    mix_value = mix_rows.astype(jnp.float32)
    gate_pre = jnp.dot(token_rows, w_gate, preferred_element_type=jnp.float32)
    up_pre = jnp.dot(token_rows, w_up, preferred_element_type=jnp.float32)
    gate_sig = jax.nn.sigmoid(gate_pre)
    active = gate_pre * gate_sig
    hidden = (active * up_pre).astype(jnp.bfloat16)
    back_hidden = jnp.dot(output_rows, w_down.T, preferred_element_type=jnp.float32)
    mix_part = lax.optimization_barrier(jnp.sum(hidden.astype(jnp.float32) * back_hidden, axis=1))
    scaled = mix_value[:, None] * back_hidden
    gate_back = (scaled * up_pre * gate_sig * (1.0 + gate_pre * (1.0 - gate_sig))).astype(jnp.bfloat16)
    up_back = (scaled * active).astype(jnp.bfloat16)
    out_scaled = (mix_value[:, None] * output_rows.astype(jnp.float32)).astype(jnp.bfloat16)
    gate_grad = jnp.dot(token_rows.T, gate_back, preferred_element_type=jnp.float32).astype(jnp.bfloat16)
    up_grad = jnp.dot(token_rows.T, up_back, preferred_element_type=jnp.float32).astype(jnp.bfloat16)
    down_grad = jnp.dot(hidden.T, out_scaled, preferred_element_type=jnp.float32).astype(jnp.bfloat16)
    slots = token_rows.shape[0]
    group = FF // N_TP
    gate_blocks = gate_back.astype(jnp.float32).reshape(slots, N_TP, group)
    up_blocks = up_back.astype(jnp.float32).reshape(slots, N_TP, group)
    terms = jnp.einsum('rtf,dtf->trd', gate_blocks, w_gate.astype(jnp.float32).reshape(D, N_TP, group))
    terms = terms + jnp.einsum('rtf,dtf->trd', up_blocks, w_up.astype(jnp.float32).reshape(D, N_TP, group))
    rounded = lax.optimization_barrier(terms.astype(jnp.bfloat16)).astype(jnp.float32)
    token_slots = lax.optimization_barrier(jnp.sum(rounded, axis=0)).astype(jnp.bfloat16)
    return (gate_grad, up_grad, down_grad, token_slots, mix_part)

def to_experts(rows):
    shaped = rows.reshape((N_EP, EXPERTS, CAP) + rows.shape[2:])
    return jnp.swapaxes(shaped, 0, 1).reshape((EXPERTS, N_EP * CAP) + rows.shape[2:])

def to_home(rows):
    shaped = rows.reshape((EXPERTS, N_EP, CAP) + rows.shape[2:])
    return jnp.swapaxes(shaped, 0, 1).reshape((N_EP, EXPERTS * CAP) + rows.shape[2:])

def reference(tokens, routes, router_matrix, cotangent, gate_proj, up_proj, down_proj):
    entries = TOK_DEV * TOP
    home_routes = routes.reshape(N_EP, entries)
    places, filler = jax.vmap(lambda flat: slot_places(flat, EXPERTS, CAP))(home_routes)
    occupied = filler < entries
    offsets = (jnp.arange(N_EP, dtype=jnp.int32) * TOK_DEV)[:, None]
    source = (jnp.where(occupied, filler // TOP, 0) + offsets).astype(jnp.int32)
    entry_src = (jnp.where(occupied, filler, 0) + offsets * TOP).astype(jnp.int32)
    logits = jnp.dot(tokens, router_matrix, preferred_element_type=jnp.float32)
    picked = routes[:, :, None] == jnp.arange(EXPERTS, dtype=jnp.int32)[None, None, :]
    chosen = lax.optimization_barrier(jnp.sum(jnp.where(picked, logits[:, None, :], jnp.float32(0.0)), axis=2))
    mixing = jax.nn.sigmoid(chosen - chosen[:, ::-1])
    token_slots = jnp.where(occupied[:, :, None], tokens[source], jnp.zeros((), jnp.bfloat16))
    output_slots = jnp.where(occupied[:, :, None], cotangent[source], jnp.zeros((), jnp.bfloat16))
    mix_slots = jnp.where(occupied, mixing.reshape(-1)[entry_src], jnp.float32(0.0)).astype(jnp.bfloat16)
    results = lax.map(expert_pass, (to_experts(token_slots), to_experts(output_slots), to_experts(mix_slots), gate_proj, up_proj, down_proj))
    gate_grad, up_grad, down_grad, back_slots, back_mix = results
    pick_rows = jax.vmap(lambda rows, where_at: rows[where_at])
    token_part = lax.optimization_barrier(jnp.sum(pick_rows(to_home(back_slots), places).reshape(TOKENS, TOP, D).astype(jnp.float32), axis=1))
    mixing_grad = pick_rows(to_home(back_mix), places).reshape(TOKENS, TOP)
    pairwise = mixing[:, 0] * mixing[:, 1]
    logit_grad = pairwise[:, None] * (mixing_grad - mixing_grad[:, ::-1])
    route_grad = lax.optimization_barrier(jnp.sum(jnp.where(picked, logit_grad[:, :, None], jnp.float32(0.0)), axis=1))
    router_path = jnp.dot(route_grad, router_matrix.astype(jnp.float32).T, precision=lax.Precision.HIGHEST)
    token_grad = (token_part + router_path).astype(jnp.bfloat16)
    router_grad = jnp.dot(tokens.astype(jnp.float32).T, route_grad, precision=lax.Precision.HIGHEST) * (1.0 / math.sqrt(TOKENS))
    return (token_grad, mixing_grad, router_grad, gate_grad, up_grad, down_grad)
```

```python
import math

import jax
import jax.numpy as jnp
from jax import lax
from jax.experimental import pallas as pl
from jax.experimental.pallas import tpu as pltpu
from jax.sharding import PartitionSpec as P

MESH = pl.DeviceIdType.MESH
LANES = 128
DIRECT_TOKENS = False


def remote(src, dst, send, recv, ep, tp):
    return pltpu.make_async_remote_copy(
        src_ref=src,
        dst_ref=dst,
        send_sem=send,
        recv_sem=recv,
        device_id=(ep, tp),
        device_id_type=MESH,
    )


def span(start, size):
    return pl.ds(pl.multiple_of(start * size, size), size)


def dispatch_kernel(senders, rows, capacity, col, direct):
    def body(tok_ref, cot_ref, mix_ref, tok_out, cot_out, mix_out, ep_send, ep_recv, y_send, y_recv,
             c_send, c_recv, m_send, m_recv, l_sem):
        me = lax.axis_index("ep")
        tp = lax.axis_index("tp")
        row = tp // 2
        core = tp % 2
        partner = row * 2 + (1 - core)

        def seat(step, side):
            return lax.rem(row + step + rows, rows) * 2 + side

        def piece(out, block, tp_col):
            return out.at[span(block, capacity), span(tp_col, col)]

        def source(array, dest, tp_col):
            if array == 0:
                return tok_ref.at[dest, :, span(tp_col // 2, col)] if direct else tok_ref.at[dest]
            return cot_ref.at[dest]

        items = [(1, 0), (0, 0)] + [(0, j) for j in range(1, rows) if direct]
        hops = [(a, j) for a in ((1,) if direct else (0, 1)) for j in range(1, rows)]
        outs = (tok_out, cot_out)

        def ep_copy(i, dest, block):
            array, which = items[i]
            return remote(source(array, dest, seat(which, core)), piece(outs[array], block, seat(which, core)),
                          ep_send.at[i, dest], ep_recv.at[i, block], dest, tp)

        def mix_copy(dest, block):
            return remote(mix_ref.at[dest], mix_out.at[block], m_send.at[dest], m_recv.at[block], dest, tp)

        def local_copy(i):
            array, which = items[i]
            return pltpu.make_async_copy(source(array, me, seat(which, core)),
                                         piece(outs[array], me, seat(which, core)), l_sem.at[i])

        local_mix = pltpu.make_async_copy(mix_ref.at[me], mix_out.at[me], l_sem.at[len(items)])

        def y_copy(array, step, block):
            place = piece(outs[array], block, tp)
            return remote(place, place, y_send.at[array, step, block], y_recv.at[array, step, block],
                          me, seat(step, core))

        def y_arrival(array, step, block):
            place = piece(outs[array], block, seat(-step, core))
            return remote(place, place, y_send.at[array, step, block], y_recv.at[array, step, block],
                          me, seat(step, core))

        def c_copy(array, step, block):
            place = piece(outs[array], block, seat(step, core))
            return remote(place, place, c_send.at[array, step + rows, block],
                          c_recv.at[array, step + rows, block], me, partner)

        def c_arrival(array, step, block):
            place = piece(outs[array], block, seat(step, 1 - core))
            return remote(place, place, c_send.at[array, step + rows, block],
                          c_recv.at[array, step + rows, block], me, partner)

        relays = items + [(array, -step) for array, step in hops]
        for i in range(len(items)):
            local_copy(i).start()
        local_mix.start()

        def send_all(k, carry):
            dest = lax.rem(me + k, senders)
            for i in range(len(items)):
                ep_copy(i, dest, me).start()
            mix_copy(dest, me).start()
            return carry

        lax.fori_loop(1, senders, send_all, 0)
        for i in range(len(items)):
            local_copy(i).wait()
        local_mix.wait()

        def spread(block):
            for array, step in hops:
                y_copy(array, step, block).start()
            for array, step in items:
                c_copy(array, step, block).start()

        def pass_on(block):
            for array, step in hops:
                y_arrival(array, step, block).wait_recv()
                c_copy(array, -step, block).start()

        spread(me)

        def relay(k, carry):
            block = lax.rem(me + senders - k, senders)
            for i in range(len(items)):
                ep_copy(i, block, block).wait_recv()
            spread(block)
            pass_on(lax.rem(me + senders - k + 1, senders))
            return carry

        lax.fori_loop(1, senders, relay, 0)
        pass_on(lax.rem(me + 1, senders))

        def finish(k, carry):
            block = lax.rem(me + k, senders)
            for array, step in relays:
                c_arrival(array, step, block).wait_recv()
                c_copy(array, step, block).wait_send()
            for array, step in hops:
                y_copy(array, step, block).wait_send()
            return carry

        lax.fori_loop(0, senders, finish, 0)

        def finish_ep(k, carry):
            block = lax.rem(me + k, senders)
            for i in range(len(items)):
                ep_copy(i, block, me).wait_send()
            mix_copy(block, me).wait_send()
            mix_copy(block, block).wait_recv()
            return carry

        lax.fori_loop(1, senders, finish_ep, 0)

    return body


def dispatch(tok_send, cot_send, mix_send, direct):
    senders, capacity, col = cot_send.shape
    width = col * lax.axis_size("tp")
    n_rows = lax.axis_size("tp") // 2
    vmem = pl.BlockSpec(memory_space=pltpu.VMEM)
    dma = pltpu.SemaphoreType.DMA
    rows = jax.ShapeDtypeStruct((senders * capacity, width), cot_send.dtype)
    return pl.pallas_call(
        dispatch_kernel(senders, n_rows, capacity, col, direct),
        out_shape=(rows, rows, jax.ShapeDtypeStruct(mix_send.shape, mix_send.dtype)),
        in_specs=[vmem] * 3,
        out_specs=[pl.BlockSpec(memory_space=pl.ANY)] * 2 + [vmem],
        scratch_shapes=[
            dma((2 + n_rows, senders)), dma((2 + n_rows, senders)),
            dma((2, n_rows, senders)), dma((2, n_rows, senders)),
            dma((2, 2 * n_rows, senders)), dma((2, 2 * n_rows, senders)),
            dma((senders,)), dma((senders,)),
            dma((3 + n_rows,)),
        ],
        compiler_params=pltpu.CompilerParams(has_side_effects=True, vmem_limit_bytes=24 << 20),
        name="dispatch",
    )(tok_send, cot_send, mix_send)


def combine_kernel(senders, rows, capacity, col):
    def body(terms, mix_ref, out, mix_out, c_buf, y_src, y_buf, fin, mix_got, mix_all,
             c_send, c_recv, y_send, y_recv, h_send, h_recv, m_send, m_recv, t_send, t_recv):
        me = lax.axis_index("ep")
        tp = lax.axis_index("tp")
        row = tp // 2
        core = tp % 2
        partner = row * 2 + (1 - core)

        def seat(step, side):
            return lax.rem(row + step + rows, rows) * 2 + side

        def c_copy(step, block):
            return remote(terms.at[block, :, span(seat(step, 1 - core), col)], c_buf.at[step, block],
                          c_send.at[step, block], c_recv.at[step, block], me, partner)

        def y_copy(step, block):
            return remote(y_src.at[step - 1, block], y_buf.at[step - 1, block],
                          y_send.at[step, block], y_recv.at[step, block], me, seat(step, core))

        def h_copy(dest, slot):
            return remote(fin.at[dest], out.at[slot], h_send.at[dest], h_recv.at[slot], dest, tp)

        def m_copy(dest, slot):
            return remote(mix_ref.at[dest], mix_got.at[slot], m_send.at[dest], m_recv.at[slot], dest, tp)

        def order(k):
            return lax.rem(me + k, senders)

        def start(k, carry):
            for step in list(range(1, rows)) + [0]:
                c_copy(step, order(k)).start()
            return carry

        lax.fori_loop(1, senders + 1, start, 0)

        def start_mix(k, carry):
            m_copy(order(k), me).start()
            return carry

        lax.fori_loop(1, senders, start_mix, 0)
        mix_got[me] = mix_ref[me]

        def first(block):
            for step in range(1, rows):
                c_copy(step, block).wait_recv()
                y_src[step - 1, block] = (
                    terms[block, :, span(seat(step, core), col)].astype(jnp.float32)
                    + c_buf[step, block].astype(jnp.float32)
                ).astype(y_src.dtype)
                y_copy(step, block).start()

        def total(block):
            c_copy(0, block).wait_recv()
            value = terms[block, :, span(tp, col)].astype(jnp.float32) + c_buf[0, block].astype(
                jnp.float32
            )
            for step in range(1, rows):
                y_copy(step, block).wait_recv()
                value = value + y_buf[step - 1, block].astype(jnp.float32)
            return value.astype(out.dtype)

        def second(block):
            fin[block] = total(block)
            h_copy(block, me).start()

        ahead = 2

        def lead(k, carry):
            first(order(k))
            return carry

        def steady(k, carry):
            first(order(k))
            second(order(k - ahead))
            return carry

        lax.fori_loop(1, 1 + ahead, lead, 0)
        lax.fori_loop(1 + ahead, senders + 1, steady, 0)

        def last(k, carry):
            second(order(k))
            return carry

        lax.fori_loop(senders + 1 - ahead, senders, last, 0)
        out[me] = total(me)

        def mix_arrive(k, carry):
            m_copy(order(k), order(k)).wait_recv()
            return carry

        lax.fori_loop(1, senders, mix_arrive, 0)
        mix_all[0] = mix_got[...]

        def t_copy(k):
            peer = lax.rem(tp + k, 2 * rows)
            return remote(mix_got, mix_all.at[k], t_send.at[k], t_recv.at[k], me, peer)

        for k in range(1, 2 * rows):
            t_copy(k).start()

        def finish(k, carry):
            block = order(k)
            for step in range(rows):
                c_copy(step, block).wait_send()
            for step in range(1, rows):
                y_copy(step, block).wait_send()
            return carry

        lax.fori_loop(0, senders, finish, 0)

        def finish_home(k, carry):
            block = order(k)
            h_copy(block, block).wait()
            m_copy(block, block).wait_send()
            return carry

        lax.fori_loop(1, senders, finish_home, 0)
        for k in range(1, 2 * rows):
            t_copy(k).wait()
        mix_out[...] = jnp.sum(mix_all[...], axis=0)

    return body


def combine(terms, mix_part):
    senders, capacity, width = terms.shape
    col = width // lax.axis_size("tp")
    n_rows = lax.axis_size("tp") // 2
    vmem = pl.BlockSpec(memory_space=pltpu.VMEM)
    dma = pltpu.SemaphoreType.DMA
    block = (senders, capacity, col)
    return pl.pallas_call(
        combine_kernel(senders, n_rows, capacity, col),
        out_shape=(
            jax.ShapeDtypeStruct(block, terms.dtype),
            jax.ShapeDtypeStruct(mix_part.shape, mix_part.dtype),
        ),
        in_specs=[vmem] * 2,
        out_specs=[vmem] * 2,
        scratch_shapes=[
            pltpu.VMEM((n_rows,) + block, terms.dtype),
            pltpu.VMEM((n_rows - 1,) + block, terms.dtype),
            pltpu.VMEM((n_rows - 1,) + block, terms.dtype),
            pltpu.VMEM(block, terms.dtype),
            pltpu.VMEM(mix_part.shape, mix_part.dtype),
            pltpu.VMEM((2 * n_rows,) + mix_part.shape, mix_part.dtype),
            dma((n_rows, senders)), dma((n_rows, senders)),
            dma((n_rows, senders)), dma((n_rows, senders)),
            dma((senders,)), dma((senders,)),
            dma((senders,)), dma((senders,)),
            dma((2 * n_rows,)), dma((2 * n_rows,)),
        ],
        compiler_params=pltpu.CompilerParams(has_side_effects=True, vmem_limit_bytes=32 << 20),
        name="combine",
    )(terms, mix_part)


def router_sum(terms):
    senders = terms.shape[0]

    def body(src, out, got, send, recv):
        me = lax.axis_index("ep")
        tp = lax.axis_index("tp")

        def copy(dest, slot):
            return remote(src.at[dest], got.at[slot], send.at[dest], recv.at[slot], dest, tp)

        def start(k, carry):
            copy(lax.rem(me + k, senders), me).start()
            return carry

        lax.fori_loop(1, senders, start, 0)
        got[me] = src[me]

        def wait(k, carry):
            block = lax.rem(me + k, senders)
            copy(block, block).wait()
            return carry

        lax.fori_loop(1, senders, wait, 0)
        out[...] = jnp.sum(got[...], axis=0)

    vmem = pl.BlockSpec(memory_space=pltpu.VMEM)
    dma = pltpu.SemaphoreType.DMA
    return pl.pallas_call(
        body,
        out_shape=jax.ShapeDtypeStruct(terms.shape[1:], terms.dtype),
        in_specs=[vmem],
        out_specs=vmem,
        scratch_shapes=[pltpu.VMEM(terms.shape, terms.dtype), dma((senders,)), dma((senders,))],
        compiler_params=pltpu.CompilerParams(has_side_effects=True, vmem_limit_bytes=8 << 20),
        name="router_sum",
    )(terms)


def slot_places(flat_routes, experts, capacity):
    entries = flat_routes.shape[0]
    onehot = flat_routes[:, None] == jnp.arange(experts, dtype=jnp.int32)[None, :]
    index = jnp.arange(entries, dtype=jnp.int32)
    before = (index[None, :] < index[:, None]).astype(jnp.bfloat16)
    earlier = jnp.dot(before, onehot.astype(jnp.bfloat16), preferred_element_type=jnp.float32)
    rank = jnp.sum(jnp.where(onehot, earlier, 0.0), axis=1).astype(jnp.int32)
    return flat_routes * capacity + rank


def pad_lanes(rows):
    return jnp.pad(rows[:, None, :], ((0, 0), (0, 7), (0, LANES - rows.shape[1])))


def local(tokens, routes, router_matrix, cotangent, gate_proj, up_proj, down_proj):
    ep_size = lax.axis_size("ep")
    tp_size = lax.axis_size("tp")
    tp_index = lax.axis_index("tp")
    home_rows, model_width = tokens.shape
    top_count = routes.shape[1]
    experts = router_matrix.shape[1]
    capacity = home_rows * top_count * 2 // experts
    col_width = model_width // tp_size
    places = slot_places(routes.reshape(-1), experts, capacity).reshape(home_rows, top_count)
    slot_ids = jnp.arange(experts * capacity, dtype=jnp.int32)
    hits = slot_ids[:, None, None] == places.T[None, :, :]
    pick = jnp.any(hits, axis=1).astype(jnp.bfloat16)
    logits = jnp.dot(tokens, router_matrix, preferred_element_type=jnp.float32)
    picked = routes[:, :, None] == jnp.arange(experts, dtype=jnp.int32)[None, None, :]
    chosen = jnp.sum(jnp.where(picked, logits[:, None, :], 0.0), axis=2)
    mixing = jax.nn.sigmoid(chosen - chosen[:, ::-1])
    mix_send = jnp.sum(jnp.where(hits, mixing.T[None, :, :], 0.0), axis=(1, 2))
    mix_send = pad_lanes(mix_send.reshape(experts, capacity))
    if DIRECT_TOKENS:
        token_cols = lax.dynamic_slice_in_dim(
            tokens.reshape(home_rows, tp_size // 2, 2, col_width), tp_index % 2, 1, 2
        ).reshape(home_rows, model_width // 2)
    else:
        token_cols = lax.dynamic_slice_in_dim(tokens, tp_index * col_width, col_width, 1)
    token_send = jnp.dot(pick, token_cols, preferred_element_type=jnp.float32).astype(
        jnp.bfloat16
    ).reshape(experts, capacity, -1)
    output_send = jnp.dot(pick, cotangent, preferred_element_type=jnp.float32).astype(
        jnp.bfloat16
    ).reshape(experts, capacity, col_width)
    token_rows, output_rows, mix_in = dispatch(token_send, output_send, mix_send, DIRECT_TOKENS)
    senders = ep_size
    slots = senders * capacity
    mix_value = mix_in[:, 0, :capacity].reshape(slots).astype(jnp.bfloat16).astype(jnp.float32)
    w_gate = gate_proj[0]
    w_up = up_proj[0]
    w_down = down_proj[0]
    over_rows = (((0,), (0,)), ((), ()))
    over_cols = (((1,), (1,)), ((), ()))
    gate_pre = jnp.dot(token_rows, w_gate, preferred_element_type=jnp.float32)
    up_pre = jnp.dot(token_rows, w_up, preferred_element_type=jnp.float32)
    gate_sig = jax.nn.sigmoid(gate_pre)
    active = gate_pre * gate_sig
    hidden = (active * up_pre).astype(jnp.bfloat16)
    back_hidden = lax.dot_general(
        output_rows, w_down, over_cols, preferred_element_type=jnp.float32
    )
    mix_part = jnp.sum(hidden.astype(jnp.float32) * back_hidden, axis=1)
    scaled = mix_value[:, None] * back_hidden
    gate_back = (scaled * up_pre * gate_sig * (1.0 + gate_pre * (1.0 - gate_sig))).astype(
        jnp.bfloat16
    )
    up_back = (scaled * active).astype(jnp.bfloat16)
    out_scaled = (mix_value[:, None] * output_rows).astype(jnp.bfloat16)
    slot_terms = lax.dot_general(gate_back, w_gate, over_cols, preferred_element_type=jnp.float32)
    slot_terms = slot_terms + lax.dot_general(
        up_back, w_up, over_cols, preferred_element_type=jnp.float32
    )
    gate_grad = lax.dot_general(
        token_rows, gate_back, over_rows, preferred_element_type=jnp.float32
    ).astype(jnp.bfloat16)[None]
    up_grad = lax.dot_general(
        token_rows, up_back, over_rows, preferred_element_type=jnp.float32
    ).astype(jnp.bfloat16)[None]
    down_grad = lax.dot_general(
        hidden, out_scaled, over_rows, preferred_element_type=jnp.float32
    ).astype(jnp.bfloat16)[None]
    back_rows, back_mix = combine(
        slot_terms.astype(jnp.bfloat16).reshape(senders, capacity, model_width),
        pad_lanes(mix_part.reshape(senders, capacity)),
    )
    back_flat = back_rows.reshape(experts * capacity, col_width)
    over_slots = (((0,), (0,)), ((), ()))
    token_part = lax.dot_general(pick, back_flat, over_slots, preferred_element_type=jnp.float32)
    mix_flat = back_mix[:, 0, :capacity].reshape(experts * capacity)
    mixing_grad = jnp.sum(jnp.where(hits, mix_flat[:, None, None], 0.0), axis=0).T
    pairwise = mixing[:, 0] * mixing[:, 1]
    logit_grad = pairwise[:, None] * (mixing_grad - mixing_grad[:, ::-1])
    route_grad = jnp.sum(jnp.where(picked, logit_grad[:, :, None], 0.0), axis=1)
    router_cols = lax.dynamic_slice_in_dim(
        router_matrix, tp_index * col_width, col_width, 0
    ).astype(jnp.float32)
    router_path = jnp.dot(route_grad, router_cols.T, precision=lax.Precision.HIGHEST)
    token_grad = (token_part + router_path).astype(jnp.bfloat16)
    row_share = model_width // (ep_size * tp_size)
    feature_share = lax.dynamic_slice_in_dim(
        tokens.reshape(home_rows, ep_size, tp_size, row_share), tp_index, 1, 2
    )
    feature_share = feature_share.reshape(home_rows, ep_size * row_share).astype(jnp.float32)
    norm_scale = 1.0 / math.sqrt(home_rows * ep_size)
    router_terms = (
        jnp.dot(route_grad.T, feature_share, precision=lax.Precision.HIGHEST) * norm_scale
    )
    router_terms = jnp.swapaxes(router_terms.reshape(experts, ep_size, row_share), 0, 1)
    router_terms = jnp.pad(router_terms, ((0, 0), (0, 0), (0, LANES - row_share)))
    router_grad = router_sum(router_terms)[:, :row_share].T
    return (token_grad, mixing_grad, router_grad, gate_grad, up_grad, down_grad)


def solution(mesh):
    return jax.shard_map(
        local,
        mesh=mesh,
        in_specs=(
            P("ep", None),
            P("ep", None),
            P(),
            P("ep", "tp"),
            P("ep", None, "tp"),
            P("ep", None, "tp"),
            P("ep", "tp", None),
        ),
        out_specs=(
            P("ep", "tp"),
            P("ep", None),
            P(("ep", "tp"), None),
            P("ep", None, "tp"),
            P("ep", None, "tp"),
            P("ep", "tp", None),
        ),
        check_vma=False,
    )
```

```python
import math

import jax
import jax.numpy as jnp
from jax import lax
from jax.experimental import pallas as pl
from jax.experimental.pallas import tpu as pltpu
from jax.sharding import PartitionSpec as P

MESH = pl.DeviceIdType.MESH
LANES = 128


def remote(src, dst, send, recv, ep, tp):
    return pltpu.make_async_remote_copy(
        src_ref=src,
        dst_ref=dst,
        send_sem=send,
        recv_sem=recv,
        device_id=(ep, tp),
        device_id_type=MESH,
    )


def pair(me, k, size):
    if size & (size - 1):
        return lax.rem(me + k, size)
    return sum((me // bit + k // bit) % 2 * bit for bit in (1 << b for b in range(size.bit_length() - 1)))


def came(me, k, size):
    if size & (size - 1):
        return lax.rem(me + size - k, size)
    return pair(me, k, size)


def span(start, size):
    return pl.ds(pl.multiple_of(start * size, size), size)


def dispatch_kernel(senders, rows, capacity, col):
    def body(tok_ref, cot_ref, mix_ref, tok_out, cot_out, mix_out, ep_send, ep_recv, y_send, y_recv,
             c_send, c_recv, m_send, m_recv, l_sem):
        me = lax.axis_index("ep")
        tp = lax.axis_index("tp")
        row = tp // 2
        core = tp % 2
        partner = row * 2 + (1 - core)

        def seat(step, side):
            return lax.rem(row + step + rows, rows) * 2 + side

        def piece(out, block, tp_col):
            return out.at[span(block, capacity), span(tp_col, col)]

        def source(array, dest, tp_col):
            if array == 0:
                return tok_ref.at[dest, :, span(tp_col // 2, col)]
            return cot_ref.at[dest]

        far = [(1, 0), (0, 0)]
        near = far + [(0, j) for j in range(1, rows)]
        far_hops = [(a, j) for j in range(1, rows) for a in (1, 0)]
        near_hops = [(1, j) for j in range(1, rows)]
        half = max(senders // 2, 1)
        outs = (tok_out, cot_out)

        def ep_copy(i, dest, block):
            array, which = near[i]
            return remote(source(array, dest, seat(which, core)), piece(outs[array], block, seat(which, core)),
                          ep_send.at[i, dest], ep_recv.at[i, block], dest, tp)

        def mix_copy(dest, block):
            return remote(mix_ref.at[dest], mix_out.at[block], m_send.at[dest], m_recv.at[block], dest, tp)

        def local_copy(i):
            array, which = near[i]
            return pltpu.make_async_copy(source(array, me, seat(which, core)),
                                         piece(outs[array], me, seat(which, core)), l_sem.at[i])

        local_mix = pltpu.make_async_copy(mix_ref.at[me], mix_out.at[me], l_sem.at[len(near)])

        def y_copy(array, step, block):
            place = piece(outs[array], block, tp)
            return remote(place, place, y_send.at[array, step, block], y_recv.at[array, step, block],
                          me, seat(step, core))

        def y_arrival(array, step, block):
            place = piece(outs[array], block, seat(-step, core))
            return remote(place, place, y_send.at[array, step, block], y_recv.at[array, step, block],
                          me, seat(step, core))

        def c_copy(array, step, block):
            place = piece(outs[array], block, seat(step, core))
            return remote(place, place, c_send.at[array, step + rows, block],
                          c_recv.at[array, step + rows, block], me, partner)

        def c_arrival(array, step, block):
            place = piece(outs[array], block, seat(step, 1 - core))
            return remote(place, place, c_send.at[array, step + rows, block],
                          c_recv.at[array, step + rows, block], me, partner)

        relays = far + [(array, -step) for array, step in far_hops]
        near_relays = near + [(array, -step) for array, step in near_hops]

        def send_all(count):
            def step(k, carry):
                dest = pair(me, k, senders)
                for i in range(count):
                    ep_copy(i, dest, me).start()
                mix_copy(dest, me).start()
                return carry

            return step

        lax.fori_loop(1, half, send_all(len(near)), 0)
        lax.fori_loop(half, senders, send_all(len(far)), 0)
        for i in range(len(near)):
            local_copy(i).start()
        local_mix.start()
        for i in range(len(near)):
            local_copy(i).wait()
        local_mix.wait()

        def spread(block, items, hops):
            for array, step in hops:
                y_copy(array, step, block).start()
            for array, step in items:
                c_copy(array, step, block).start()

        def pass_on(block, hops):
            for array, step in hops:
                y_arrival(array, step, block).wait_recv()
                c_copy(array, -step, block).start()

        spread(me, near, near_hops)

        def relay(items, hops, past_hops):
            def step(k, carry):
                block = came(me, k, senders)
                for i in range(len(items)):
                    ep_copy(i, block, block).wait_recv()
                spread(block, items, hops)
                pass_on(came(me, k - 1, senders), past_hops)
                return carry

            return step

        lax.fori_loop(1, half, relay(near, near_hops, near_hops), 0)
        lax.fori_loop(half, min(half + 1, senders), relay(far, far_hops, near_hops), 0)
        lax.fori_loop(half + 1, senders, relay(far, far_hops, far_hops), 0)
        pass_on(came(me, senders - 1, senders), far_hops if senders > 1 else near_hops)

        def finish(through, hops):
            def step(k, carry):
                block = came(me, k, senders)
                for array, step in through:
                    c_arrival(array, step, block).wait_recv()
                    c_copy(array, step, block).wait_send()
                for array, step in hops:
                    y_copy(array, step, block).wait_send()
                return carry

            return step

        lax.fori_loop(0, half, finish(near_relays, near_hops), 0)
        lax.fori_loop(half, senders, finish(relays, far_hops), 0)

        def finish_ep(count):
            def step(k, carry):
                dest, block = pair(me, k, senders), came(me, k, senders)
                for i in range(count):
                    ep_copy(i, dest, me).wait_send()
                mix_copy(dest, me).wait_send()
                mix_copy(block, block).wait_recv()
                return carry

            return step

        lax.fori_loop(1, half, finish_ep(len(near)), 0)
        lax.fori_loop(half, senders, finish_ep(len(far)), 0)

    return body


def dispatch(tok_send, cot_send, mix_send):
    senders, capacity, col = cot_send.shape
    width = col * lax.axis_size("tp")
    n_rows = lax.axis_size("tp") // 2
    vmem = pl.BlockSpec(memory_space=pltpu.VMEM)
    dma = pltpu.SemaphoreType.DMA
    rows = jax.ShapeDtypeStruct((senders * capacity, width), cot_send.dtype)
    return pl.pallas_call(
        dispatch_kernel(senders, n_rows, capacity, col),
        out_shape=(rows, rows, jax.ShapeDtypeStruct(mix_send.shape, mix_send.dtype)),
        in_specs=[vmem] * 3,
        out_specs=[pl.BlockSpec(memory_space=pl.ANY)] * 2 + [vmem],
        scratch_shapes=[
            dma((2 + n_rows, senders)), dma((2 + n_rows, senders)),
            dma((2, n_rows, senders)), dma((2, n_rows, senders)),
            dma((2, 2 * n_rows, senders)), dma((2, 2 * n_rows, senders)),
            dma((senders,)), dma((senders,)),
            dma((3 + n_rows,)),
        ],
        compiler_params=pltpu.CompilerParams(has_side_effects=True, vmem_limit_bytes=24 << 20),
        name="dispatch",
    )(tok_send, cot_send, mix_send)


def combine_kernel(senders, rows, capacity, col):
    def body(terms, mix_ref, out, mix_out, c_buf, y_src, y_buf, fin, mix_got, mix_all,
             c_send, c_recv, y_send, y_recv, h_send, h_recv, m_send, m_recv, t_send, t_recv):
        me = lax.axis_index("ep")
        tp = lax.axis_index("tp")
        row = tp // 2
        core = tp % 2
        partner = row * 2 + (1 - core)

        def seat(step, side):
            return lax.rem(row + step + rows, rows) * 2 + side

        def c_copy(step, block):
            return remote(terms.at[block, :, span(seat(step, 1 - core), col)], c_buf.at[step, block],
                          c_send.at[step, block], c_recv.at[step, block], me, partner)

        def y_copy(step, block):
            return remote(y_src.at[step - 1, block], y_buf.at[step - 1, block],
                          y_send.at[step, block], y_recv.at[step, block], me, seat(step, core))

        def h_copy(dest, slot):
            return remote(fin.at[dest], out.at[slot], h_send.at[dest], h_recv.at[slot], dest, tp)

        def m_copy(dest, slot):
            return remote(mix_ref.at[dest], mix_got.at[slot], m_send.at[dest], m_recv.at[slot], dest, tp)

        def order(k):
            return pair(me, senders - k, senders)

        def start(k, carry):
            for step in list(range(1, rows)) + [0]:
                c_copy(step, order(k)).start()
            return carry

        lax.fori_loop(1, senders + 1, start, 0)

        def start_mix(k, carry):
            m_copy(order(k), me).start()
            return carry

        lax.fori_loop(1, senders, start_mix, 0)
        mix_got[me] = mix_ref[me]

        def first(block):
            for step in range(1, rows):
                c_copy(step, block).wait_recv()
                y_src[step - 1, block] = (
                    terms[block, :, span(seat(step, core), col)].astype(jnp.float32)
                    + c_buf[step, block].astype(jnp.float32)
                ).astype(y_src.dtype)
                y_copy(step, block).start()

        def total(block):
            c_copy(0, block).wait_recv()
            value = terms[block, :, span(tp, col)].astype(jnp.float32) + c_buf[0, block].astype(
                jnp.float32
            )
            for step in range(1, rows):
                y_copy(step, block).wait_recv()
                value = value + y_buf[step - 1, block].astype(jnp.float32)
            return value.astype(out.dtype)

        def second(block):
            fin[block] = total(block)
            h_copy(block, me).start()

        ahead = 2

        def lead(k, carry):
            first(order(k))
            return carry

        def steady(k, carry):
            first(order(k))
            second(order(k - ahead))
            return carry

        lax.fori_loop(1, 1 + ahead, lead, 0)
        lax.fori_loop(1 + ahead, senders + 1, steady, 0)

        def last(k, carry):
            second(order(k))
            return carry

        lax.fori_loop(senders + 1 - ahead, senders, last, 0)
        out[me] = total(me)

        def mix_arrive(k, carry):
            m_copy(order(k), order(k)).wait_recv()
            return carry

        lax.fori_loop(1, senders, mix_arrive, 0)
        mix_all[0] = mix_got[...]

        def t_copy(k):
            peer = lax.rem(tp + k, 2 * rows)
            return remote(mix_got, mix_all.at[k], t_send.at[k], t_recv.at[k], me, peer)

        for k in range(1, 2 * rows):
            t_copy(k).start()

        def finish(k, carry):
            block = order(k)
            for step in range(rows):
                c_copy(step, block).wait_send()
            for step in range(1, rows):
                y_copy(step, block).wait_send()
            return carry

        lax.fori_loop(0, senders, finish, 0)

        def finish_home(k, carry):
            block = order(k)
            h_copy(block, block).wait()
            m_copy(block, block).wait_send()
            return carry

        lax.fori_loop(1, senders, finish_home, 0)
        for k in range(1, 2 * rows):
            t_copy(k).wait()
        mix_out[...] = jnp.sum(mix_all[...], axis=0)

    return body


def combine(terms, mix_part):
    senders, capacity, width = terms.shape
    col = width // lax.axis_size("tp")
    n_rows = lax.axis_size("tp") // 2
    vmem = pl.BlockSpec(memory_space=pltpu.VMEM)
    dma = pltpu.SemaphoreType.DMA
    block = (senders, capacity, col)
    return pl.pallas_call(
        combine_kernel(senders, n_rows, capacity, col),
        out_shape=(
            jax.ShapeDtypeStruct(block, terms.dtype),
            jax.ShapeDtypeStruct(mix_part.shape, mix_part.dtype),
        ),
        in_specs=[vmem] * 2,
        out_specs=[vmem] * 2,
        scratch_shapes=[
            pltpu.VMEM((n_rows,) + block, terms.dtype),
            pltpu.VMEM((n_rows - 1,) + block, terms.dtype),
            pltpu.VMEM((n_rows - 1,) + block, terms.dtype),
            pltpu.VMEM(block, terms.dtype),
            pltpu.VMEM(mix_part.shape, mix_part.dtype),
            pltpu.VMEM((2 * n_rows,) + mix_part.shape, mix_part.dtype),
            dma((n_rows, senders)), dma((n_rows, senders)),
            dma((n_rows, senders)), dma((n_rows, senders)),
            dma((senders,)), dma((senders,)),
            dma((senders,)), dma((senders,)),
            dma((2 * n_rows,)), dma((2 * n_rows,)),
        ],
        compiler_params=pltpu.CompilerParams(has_side_effects=True, vmem_limit_bytes=32 << 20),
        name="combine",
    )(terms, mix_part)


def router_sum(terms):
    senders = terms.shape[0]

    def body(src, out, got, send, recv):
        me = lax.axis_index("ep")
        tp = lax.axis_index("tp")

        def copy(dest, slot):
            return remote(src.at[dest], got.at[slot], send.at[dest], recv.at[slot], dest, tp)

        def start(k, carry):
            copy(lax.rem(me + k, senders), me).start()
            return carry

        lax.fori_loop(1, senders, start, 0)
        got[me] = src[me]

        def wait(k, carry):
            block = lax.rem(me + k, senders)
            copy(block, block).wait()
            return carry

        lax.fori_loop(1, senders, wait, 0)
        out[...] = jnp.sum(got[...], axis=0)

    vmem = pl.BlockSpec(memory_space=pltpu.VMEM)
    dma = pltpu.SemaphoreType.DMA
    return pl.pallas_call(
        body,
        out_shape=jax.ShapeDtypeStruct(terms.shape[1:], terms.dtype),
        in_specs=[vmem],
        out_specs=vmem,
        scratch_shapes=[pltpu.VMEM(terms.shape, terms.dtype), dma((senders,)), dma((senders,))],
        compiler_params=pltpu.CompilerParams(has_side_effects=True, vmem_limit_bytes=8 << 20),
        name="router_sum",
    )(terms)


def slot_places(flat_routes, experts, capacity):
    entries = flat_routes.shape[0]
    onehot = flat_routes[:, None] == jnp.arange(experts, dtype=jnp.int32)[None, :]
    index = jnp.arange(entries, dtype=jnp.int32)
    before = (index[None, :] < index[:, None]).astype(jnp.bfloat16)
    earlier = jnp.dot(before, onehot.astype(jnp.bfloat16), preferred_element_type=jnp.float32)
    rank = jnp.sum(jnp.where(onehot, earlier, 0.0), axis=1).astype(jnp.int32)
    return flat_routes * capacity + rank


def pad_lanes(rows):
    return jnp.pad(rows[:, None, :], ((0, 0), (0, 7), (0, LANES - rows.shape[1])))


def local(tokens, routes, router_matrix, cotangent, gate_proj, up_proj, down_proj):
    ep_size = lax.axis_size("ep")
    tp_size = lax.axis_size("tp")
    tp_index = lax.axis_index("tp")
    home_rows, model_width = tokens.shape
    top_count = routes.shape[1]
    experts = router_matrix.shape[1]
    capacity = home_rows * top_count * 2 // experts
    col_width = model_width // tp_size
    places = slot_places(routes.reshape(-1), experts, capacity).reshape(home_rows, top_count)
    slot_ids = jnp.arange(experts * capacity, dtype=jnp.int32)
    hits = slot_ids[:, None, None] == places.T[None, :, :]
    pick = jnp.any(hits, axis=1).astype(jnp.bfloat16)
    logits = jnp.dot(tokens, router_matrix, preferred_element_type=jnp.float32)
    picked = routes[:, :, None] == jnp.arange(experts, dtype=jnp.int32)[None, None, :]
    chosen = jnp.sum(jnp.where(picked, logits[:, None, :], 0.0), axis=2)
    mixing = jax.nn.sigmoid(chosen - chosen[:, ::-1])
    mix_send = jnp.sum(jnp.where(hits, mixing.T[None, :, :], 0.0), axis=(1, 2))
    mix_send = pad_lanes(mix_send.reshape(experts, capacity))
    token_cols = lax.dynamic_slice_in_dim(
        tokens.reshape(home_rows, tp_size // 2, 2, col_width), tp_index % 2, 1, 2
    ).reshape(home_rows, model_width // 2)
    token_send = jnp.dot(pick, token_cols, preferred_element_type=jnp.float32).astype(
        jnp.bfloat16
    ).reshape(experts, capacity, -1)
    output_send = jnp.dot(pick, cotangent, preferred_element_type=jnp.float32).astype(
        jnp.bfloat16
    ).reshape(experts, capacity, col_width)
    token_rows, output_rows, mix_in = dispatch(token_send, output_send, mix_send)
    senders = ep_size
    slots = senders * capacity
    mix_value = mix_in[:, 0, :capacity].reshape(slots).astype(jnp.bfloat16).astype(jnp.float32)
    w_gate = gate_proj[0]
    w_up = up_proj[0]
    w_down = down_proj[0]
    over_rows = (((0,), (0,)), ((), ()))
    over_cols = (((1,), (1,)), ((), ()))
    gate_pre = jnp.dot(token_rows, w_gate, preferred_element_type=jnp.float32)
    up_pre = jnp.dot(token_rows, w_up, preferred_element_type=jnp.float32)
    gate_sig = jax.nn.sigmoid(gate_pre)
    active = gate_pre * gate_sig
    hidden = (active * up_pre).astype(jnp.bfloat16)
    back_hidden = lax.dot_general(
        output_rows, w_down, over_cols, preferred_element_type=jnp.float32
    )
    mix_part = jnp.sum(hidden.astype(jnp.float32) * back_hidden, axis=1)
    scaled = mix_value[:, None] * back_hidden
    gate_back = (scaled * up_pre * gate_sig * (1.0 + gate_pre * (1.0 - gate_sig))).astype(
        jnp.bfloat16
    )
    up_back = (scaled * active).astype(jnp.bfloat16)
    out_scaled = (mix_value[:, None] * output_rows).astype(jnp.bfloat16)
    slot_terms = lax.dot_general(gate_back, w_gate, over_cols, preferred_element_type=jnp.float32)
    slot_terms = slot_terms + lax.dot_general(
        up_back, w_up, over_cols, preferred_element_type=jnp.float32
    )
    gate_grad = lax.dot_general(
        token_rows, gate_back, over_rows, preferred_element_type=jnp.float32
    ).astype(jnp.bfloat16)[None]
    up_grad = lax.dot_general(
        token_rows, up_back, over_rows, preferred_element_type=jnp.float32
    ).astype(jnp.bfloat16)[None]
    down_grad = lax.dot_general(
        hidden, out_scaled, over_rows, preferred_element_type=jnp.float32
    ).astype(jnp.bfloat16)[None]
    back_rows, back_mix = combine(
        slot_terms.astype(jnp.bfloat16).reshape(senders, capacity, model_width),
        pad_lanes(mix_part.reshape(senders, capacity)),
    )
    back_flat = back_rows.reshape(experts * capacity, col_width)
    over_slots = (((0,), (0,)), ((), ()))
    token_part = lax.dot_general(pick, back_flat, over_slots, preferred_element_type=jnp.float32)
    mix_flat = back_mix[:, 0, :capacity].reshape(experts * capacity)
    mixing_grad = jnp.sum(jnp.where(hits, mix_flat[:, None, None], 0.0), axis=0).T
    pairwise = mixing[:, 0] * mixing[:, 1]
    logit_grad = pairwise[:, None] * (mixing_grad - mixing_grad[:, ::-1])
    route_grad = jnp.sum(jnp.where(picked, logit_grad[:, :, None], 0.0), axis=1)
    router_cols = lax.dynamic_slice_in_dim(
        router_matrix, tp_index * col_width, col_width, 0
    ).astype(jnp.float32)
    router_path = jnp.dot(route_grad, router_cols.T, precision=lax.Precision.HIGHEST)
    token_grad = (token_part + router_path).astype(jnp.bfloat16)
    row_share = model_width // (ep_size * tp_size)
    feature_share = lax.dynamic_slice_in_dim(
        tokens.reshape(home_rows, ep_size, tp_size, row_share), tp_index, 1, 2
    )
    feature_share = feature_share.reshape(home_rows, ep_size * row_share).astype(jnp.float32)
    norm_scale = 1.0 / math.sqrt(home_rows * ep_size)
    router_terms = (
        jnp.dot(route_grad.T, feature_share, precision=lax.Precision.HIGHEST) * norm_scale
    )
    router_terms = jnp.swapaxes(router_terms.reshape(experts, ep_size, row_share), 0, 1)
    router_terms = jnp.pad(router_terms, ((0, 0), (0, 0), (0, LANES - row_share)))
    router_grad = router_sum(router_terms)[:, :row_share].T
    return (token_grad, mixing_grad, router_grad, gate_grad, up_grad, down_grad)


def solution(mesh):
    return jax.shard_map(
        local,
        mesh=mesh,
        in_specs=(
            P("ep", None),
            P("ep", None),
            P(),
            P("ep", "tp"),
            P("ep", None, "tp"),
            P("ep", None, "tp"),
            P("ep", "tp", None),
        ),
        out_specs=(
            P("ep", "tp"),
            P("ep", None),
            P(("ep", "tp"), None),
            P("ep", None, "tp"),
            P("ep", None, "tp"),
            P("ep", "tp", None),
        ),
        check_vma=False,
    )
```

```python
import math

import jax
import jax.numpy as jnp
from jax import lax
from jax.experimental import pallas as pl
from jax.experimental.pallas import tpu as pltpu
from jax.sharding import PartitionSpec as P

MESH = pl.DeviceIdType.MESH
LANES = 128


def remote(src, dst, send, recv, ep, tp):
    return pltpu.make_async_remote_copy(
        src_ref=src,
        dst_ref=dst,
        send_sem=send,
        recv_sem=recv,
        device_id=(ep, tp),
        device_id_type=MESH,
    )


def pair(me, k, size):
    if size & (size - 1):
        return lax.rem(me + k, size)
    return sum((me // bit + k // bit) % 2 * bit for bit in (1 << b for b in range(size.bit_length() - 1)))


def came(me, k, size):
    if size & (size - 1):
        return lax.rem(me + size - k, size)
    return pair(me, k, size)


def greet(me, tp, senders, peers):
    barrier = pltpu.get_barrier_semaphore()

    def hello(k, carry):
        pl.semaphore_signal(barrier, inc=1, device_id=(pair(me, k, senders), tp), device_id_type=MESH)
        return carry

    lax.fori_loop(1, senders, hello, 0)
    for peer in peers:
        pl.semaphore_signal(barrier, inc=1, device_id=(me, peer), device_id_type=MESH)
    pl.semaphore_wait(barrier, senders - 1 + len(peers))


def span(start, size):
    return pl.ds(pl.multiple_of(start * size, size), size)


def dispatch_kernel(senders, rows, capacity, col):
    def body(tok_ref, cot_ref, mix_ref, tok_out, cot_out, mix_out, ep_send, ep_recv, y_send, y_recv,
             c_send, c_recv, m_send, m_recv, l_sem):
        me = lax.axis_index("ep")
        tp = lax.axis_index("tp")
        row = tp // 2
        core = tp % 2
        partner = row * 2 + (1 - core)

        def seat(step, side):
            return lax.rem(row + step + rows, rows) * 2 + side

        greet(me, tp, senders, [partner] + [seat(j, core) for j in range(1, rows)])

        def piece(out, block, tp_col):
            return out.at[span(block, capacity), span(tp_col, col)]

        def source(array, dest, tp_col):
            if array == 0:
                return tok_ref.at[dest, :, span(tp_col // 2, col)]
            return cot_ref.at[dest]

        far = [(1, 0), (0, 0)]
        near = far + [(0, j) for j in range(1, rows)]
        far_hops = [(a, j) for j in range(1, rows) for a in (1, 0)]
        near_hops = [(1, j) for j in range(1, rows)]
        half = max(senders // 2, 1)
        outs = (tok_out, cot_out)

        def ep_copy(i, dest, block):
            array, which = near[i]
            return remote(source(array, dest, seat(which, core)), piece(outs[array], block, seat(which, core)),
                          ep_send.at[i, dest], ep_recv.at[i, block], dest, tp)

        def mix_copy(dest, block):
            return remote(mix_ref.at[dest], mix_out.at[block], m_send.at[dest], m_recv.at[block], dest, tp)

        def local_copy(i):
            array, which = near[i]
            return pltpu.make_async_copy(source(array, me, seat(which, core)),
                                         piece(outs[array], me, seat(which, core)), l_sem.at[i])

        local_mix = pltpu.make_async_copy(mix_ref.at[me], mix_out.at[me], l_sem.at[len(near)])

        def y_copy(array, step, block):
            place = piece(outs[array], block, tp)
            return remote(place, place, y_send.at[array, step, block], y_recv.at[array, step, block],
                          me, seat(step, core))

        def y_arrival(array, step, block):
            place = piece(outs[array], block, seat(-step, core))
            return remote(place, place, y_send.at[array, step, block], y_recv.at[array, step, block],
                          me, seat(step, core))

        def c_copy(array, step, block):
            place = piece(outs[array], block, seat(step, core))
            return remote(place, place, c_send.at[array, step + rows, block],
                          c_recv.at[array, step + rows, block], me, partner)

        def c_arrival(array, step, block):
            place = piece(outs[array], block, seat(step, 1 - core))
            return remote(place, place, c_send.at[array, step + rows, block],
                          c_recv.at[array, step + rows, block], me, partner)

        relays = far + [(array, -step) for array, step in far_hops]
        near_relays = near + [(array, -step) for array, step in near_hops]

        def send_all(count):
            def step(k, carry):
                dest = pair(me, k, senders)
                for i in range(count):
                    ep_copy(i, dest, me).start()
                mix_copy(dest, me).start()
                return carry

            return step

        lax.fori_loop(1, half, send_all(len(near)), 0)
        lax.fori_loop(half, senders, send_all(len(far)), 0)
        for i in range(len(near)):
            local_copy(i).start()
        local_mix.start()
        for i in range(len(near)):
            local_copy(i).wait()
        local_mix.wait()

        def spread(block, items, hops):
            for array, step in hops:
                y_copy(array, step, block).start()
            for array, step in items:
                c_copy(array, step, block).start()

        def pass_on(block, hops):
            for array, step in hops:
                y_arrival(array, step, block).wait_recv()
                c_copy(array, -step, block).start()

        spread(me, near, near_hops)

        def relay(items, hops, past_hops):
            def step(k, carry):
                block = came(me, k, senders)
                for i in range(len(items)):
                    ep_copy(i, block, block).wait_recv()
                spread(block, items, hops)
                pass_on(came(me, k - 1, senders), past_hops)
                return carry

            return step

        lax.fori_loop(1, half, relay(near, near_hops, near_hops), 0)
        lax.fori_loop(half, min(half + 1, senders), relay(far, far_hops, near_hops), 0)
        lax.fori_loop(half + 1, senders, relay(far, far_hops, far_hops), 0)
        pass_on(came(me, senders - 1, senders), far_hops if senders > 1 else near_hops)

        def finish(through, hops):
            def step(k, carry):
                block = came(me, k, senders)
                for array, step in through:
                    c_arrival(array, step, block).wait_recv()
                    c_copy(array, step, block).wait_send()
                for array, step in hops:
                    y_copy(array, step, block).wait_send()
                return carry

            return step

        lax.fori_loop(0, half, finish(near_relays, near_hops), 0)
        lax.fori_loop(half, senders, finish(relays, far_hops), 0)

        def finish_ep(count):
            def step(k, carry):
                dest, block = pair(me, k, senders), came(me, k, senders)
                for i in range(count):
                    ep_copy(i, dest, me).wait_send()
                mix_copy(dest, me).wait_send()
                mix_copy(block, block).wait_recv()
                return carry

            return step

        lax.fori_loop(1, half, finish_ep(len(near)), 0)
        lax.fori_loop(half, senders, finish_ep(len(far)), 0)

    return body


def dispatch(tok_send, cot_send, mix_send):
    senders, capacity, col = cot_send.shape
    width = col * lax.axis_size("tp")
    n_rows = lax.axis_size("tp") // 2
    vmem = pl.BlockSpec(memory_space=pltpu.VMEM)
    dma = pltpu.SemaphoreType.DMA
    rows = jax.ShapeDtypeStruct((senders * capacity, width), cot_send.dtype)
    return pl.pallas_call(
        dispatch_kernel(senders, n_rows, capacity, col),
        out_shape=(rows, rows, jax.ShapeDtypeStruct(mix_send.shape, mix_send.dtype)),
        in_specs=[vmem] * 3,
        out_specs=[pl.BlockSpec(memory_space=pl.ANY)] * 2 + [vmem],
        scratch_shapes=[
            dma((2 + n_rows, senders)), dma((2 + n_rows, senders)),
            dma((2, n_rows, senders)), dma((2, n_rows, senders)),
            dma((2, 2 * n_rows, senders)), dma((2, 2 * n_rows, senders)),
            dma((senders,)), dma((senders,)),
            dma((3 + n_rows,)),
        ],
        compiler_params=pltpu.CompilerParams(has_side_effects=True, collective_id=0, vmem_limit_bytes=24 << 20),
        name="dispatch",
    )(tok_send, cot_send, mix_send)


def combine_kernel(senders, rows, capacity, col):
    def body(terms, mix_ref, out, mix_out, c_buf, y_src, y_buf, fin, mix_got, mix_all,
             c_send, c_recv, y_send, y_recv, h_send, h_recv, m_send, m_recv, t_send, t_recv):
        me = lax.axis_index("ep")
        tp = lax.axis_index("tp")
        row = tp // 2
        core = tp % 2
        partner = row * 2 + (1 - core)

        def seat(step, side):
            return lax.rem(row + step + rows, rows) * 2 + side

        greet(me, tp, senders, [lax.rem(tp + k, 2 * rows) for k in range(1, 2 * rows)])

        def c_copy(step, block):
            return remote(terms.at[block, :, span(seat(step, 1 - core), col)], c_buf.at[step, block],
                          c_send.at[step, block], c_recv.at[step, block], me, partner)

        def y_copy(step, block):
            return remote(y_src.at[step - 1, block], y_buf.at[step - 1, block],
                          y_send.at[step, block], y_recv.at[step, block], me, seat(step, core))

        def h_copy(dest, slot):
            return remote(fin.at[dest], out.at[slot], h_send.at[dest], h_recv.at[slot], dest, tp)

        def m_copy(dest, slot):
            return remote(mix_ref.at[dest], mix_got.at[slot], m_send.at[dest], m_recv.at[slot], dest, tp)

        def order(k):
            return pair(me, senders - k, senders)

        def start(k, carry):
            for step in list(range(1, rows)) + [0]:
                c_copy(step, order(k)).start()
            return carry

        lax.fori_loop(1, senders + 1, start, 0)

        def start_mix(k, carry):
            m_copy(order(k), me).start()
            return carry

        lax.fori_loop(1, senders, start_mix, 0)
        mix_got[me] = mix_ref[me]

        def first(block):
            for step in range(1, rows):
                c_copy(step, block).wait_recv()
                y_src[step - 1, block] = (
                    terms[block, :, span(seat(step, core), col)].astype(jnp.float32)
                    + c_buf[step, block].astype(jnp.float32)
                ).astype(y_src.dtype)
                y_copy(step, block).start()

        def total(block):
            c_copy(0, block).wait_recv()
            value = terms[block, :, span(tp, col)].astype(jnp.float32) + c_buf[0, block].astype(
                jnp.float32
            )
            for step in range(1, rows):
                y_copy(step, block).wait_recv()
                value = value + y_buf[step - 1, block].astype(jnp.float32)
            return value.astype(out.dtype)

        def second(block):
            fin[block] = total(block)
            h_copy(block, me).start()

        ahead = 2

        def lead(k, carry):
            first(order(k))
            return carry

        def steady(k, carry):
            first(order(k))
            second(order(k - ahead))
            return carry

        lax.fori_loop(1, 1 + ahead, lead, 0)
        lax.fori_loop(1 + ahead, senders + 1, steady, 0)

        def last(k, carry):
            second(order(k))
            return carry

        lax.fori_loop(senders + 1 - ahead, senders, last, 0)
        out[me] = total(me)

        def mix_arrive(k, carry):
            m_copy(order(k), order(k)).wait_recv()
            return carry

        lax.fori_loop(1, senders, mix_arrive, 0)
        mix_all[0] = mix_got[...]

        def t_copy(k):
            peer = lax.rem(tp + k, 2 * rows)
            return remote(mix_got, mix_all.at[k], t_send.at[k], t_recv.at[k], me, peer)

        for k in range(1, 2 * rows):
            t_copy(k).start()

        def finish(k, carry):
            block = order(k)
            for step in range(rows):
                c_copy(step, block).wait_send()
            for step in range(1, rows):
                y_copy(step, block).wait_send()
            return carry

        lax.fori_loop(0, senders, finish, 0)

        def finish_home(k, carry):
            block = order(k)
            h_copy(block, block).wait()
            m_copy(block, block).wait_send()
            return carry

        lax.fori_loop(1, senders, finish_home, 0)
        for k in range(1, 2 * rows):
            t_copy(k).wait()
        mix_out[...] = jnp.sum(mix_all[...], axis=0)

    return body


def combine(terms, mix_part):
    senders, capacity, width = terms.shape
    col = width // lax.axis_size("tp")
    n_rows = lax.axis_size("tp") // 2
    vmem = pl.BlockSpec(memory_space=pltpu.VMEM)
    dma = pltpu.SemaphoreType.DMA
    block = (senders, capacity, col)
    return pl.pallas_call(
        combine_kernel(senders, n_rows, capacity, col),
        out_shape=(
            jax.ShapeDtypeStruct(block, terms.dtype),
            jax.ShapeDtypeStruct(mix_part.shape, mix_part.dtype),
        ),
        in_specs=[vmem] * 2,
        out_specs=[vmem] * 2,
        scratch_shapes=[
            pltpu.VMEM((n_rows,) + block, terms.dtype),
            pltpu.VMEM((n_rows - 1,) + block, terms.dtype),
            pltpu.VMEM((n_rows - 1,) + block, terms.dtype),
            pltpu.VMEM(block, terms.dtype),
            pltpu.VMEM(mix_part.shape, mix_part.dtype),
            pltpu.VMEM((2 * n_rows,) + mix_part.shape, mix_part.dtype),
            dma((n_rows, senders)), dma((n_rows, senders)),
            dma((n_rows, senders)), dma((n_rows, senders)),
            dma((senders,)), dma((senders,)),
            dma((senders,)), dma((senders,)),
            dma((2 * n_rows,)), dma((2 * n_rows,)),
        ],
        compiler_params=pltpu.CompilerParams(has_side_effects=True, collective_id=1, vmem_limit_bytes=32 << 20),
        name="combine",
    )(terms, mix_part)


def router_sum(terms):
    senders = terms.shape[0]

    def body(src, out, got, send, recv):
        me = lax.axis_index("ep")
        tp = lax.axis_index("tp")

        greet(me, tp, senders, [])

        def copy(dest, slot):
            return remote(src.at[dest], got.at[slot], send.at[dest], recv.at[slot], dest, tp)

        def start(k, carry):
            copy(lax.rem(me + k, senders), me).start()
            return carry

        lax.fori_loop(1, senders, start, 0)
        got[me] = src[me]

        def wait(k, carry):
            block = lax.rem(me + k, senders)
            copy(block, block).wait()
            return carry

        lax.fori_loop(1, senders, wait, 0)
        out[...] = jnp.sum(got[...], axis=0)

    vmem = pl.BlockSpec(memory_space=pltpu.VMEM)
    dma = pltpu.SemaphoreType.DMA
    return pl.pallas_call(
        body,
        out_shape=jax.ShapeDtypeStruct(terms.shape[1:], terms.dtype),
        in_specs=[vmem],
        out_specs=vmem,
        scratch_shapes=[pltpu.VMEM(terms.shape, terms.dtype), dma((senders,)), dma((senders,))],
        compiler_params=pltpu.CompilerParams(has_side_effects=True, collective_id=2, vmem_limit_bytes=8 << 20),
        name="router_sum",
    )(terms)


def slot_places(flat_routes, experts, capacity):
    entries = flat_routes.shape[0]
    onehot = flat_routes[:, None] == jnp.arange(experts, dtype=jnp.int32)[None, :]
    index = jnp.arange(entries, dtype=jnp.int32)
    before = (index[None, :] < index[:, None]).astype(jnp.bfloat16)
    earlier = jnp.dot(before, onehot.astype(jnp.bfloat16), preferred_element_type=jnp.float32)
    rank = jnp.sum(jnp.where(onehot, earlier, 0.0), axis=1).astype(jnp.int32)
    return flat_routes * capacity + rank


def pad_lanes(rows):
    return jnp.pad(rows[:, None, :], ((0, 0), (0, 7), (0, LANES - rows.shape[1])))


def local(tokens, routes, router_matrix, cotangent, gate_proj, up_proj, down_proj):
    ep_size = lax.axis_size("ep")
    tp_size = lax.axis_size("tp")
    tp_index = lax.axis_index("tp")
    home_rows, model_width = tokens.shape
    top_count = routes.shape[1]
    experts = router_matrix.shape[1]
    capacity = home_rows * top_count * 2 // experts
    col_width = model_width // tp_size
    places = slot_places(routes.reshape(-1), experts, capacity).reshape(home_rows, top_count)
    slot_ids = jnp.arange(experts * capacity, dtype=jnp.int32)
    hits = slot_ids[:, None, None] == places.T[None, :, :]
    pick = jnp.any(hits, axis=1).astype(jnp.bfloat16)
    logits = jnp.dot(tokens, router_matrix, preferred_element_type=jnp.float32)
    picked = routes[:, :, None] == jnp.arange(experts, dtype=jnp.int32)[None, None, :]
    chosen = jnp.sum(jnp.where(picked, logits[:, None, :], 0.0), axis=2)
    mixing = jax.nn.sigmoid(chosen - chosen[:, ::-1])
    mix_send = jnp.sum(jnp.where(hits, mixing.T[None, :, :], 0.0), axis=(1, 2))
    mix_send = pad_lanes(mix_send.reshape(experts, capacity))
    token_cols = lax.dynamic_slice_in_dim(
        tokens.reshape(home_rows, tp_size // 2, 2, col_width), tp_index % 2, 1, 2
    ).reshape(home_rows, model_width // 2)
    token_send = jnp.dot(pick, token_cols, preferred_element_type=jnp.float32).astype(
        jnp.bfloat16
    ).reshape(experts, capacity, -1)
    output_send = jnp.dot(pick, cotangent, preferred_element_type=jnp.float32).astype(
        jnp.bfloat16
    ).reshape(experts, capacity, col_width)
    token_rows, output_rows, mix_in = dispatch(token_send, output_send, mix_send)
    senders = ep_size
    slots = senders * capacity
    mix_value = mix_in[:, 0, :capacity].reshape(slots).astype(jnp.bfloat16).astype(jnp.float32)
    w_gate = gate_proj[0]
    w_up = up_proj[0]
    w_down = down_proj[0]
    over_rows = (((0,), (0,)), ((), ()))
    over_cols = (((1,), (1,)), ((), ()))
    gate_pre = jnp.dot(token_rows, w_gate, preferred_element_type=jnp.float32)
    up_pre = jnp.dot(token_rows, w_up, preferred_element_type=jnp.float32)
    gate_sig = jax.nn.sigmoid(gate_pre)
    active = gate_pre * gate_sig
    hidden = (active * up_pre).astype(jnp.bfloat16)
    back_hidden = lax.dot_general(
        output_rows, w_down, over_cols, preferred_element_type=jnp.float32
    )
    mix_part = jnp.sum(hidden.astype(jnp.float32) * back_hidden, axis=1)
    scaled = mix_value[:, None] * back_hidden
    gate_back = (scaled * up_pre * gate_sig * (1.0 + gate_pre * (1.0 - gate_sig))).astype(
        jnp.bfloat16
    )
    up_back = (scaled * active).astype(jnp.bfloat16)
    out_scaled = (mix_value[:, None] * output_rows).astype(jnp.bfloat16)
    slot_terms = lax.dot_general(gate_back, w_gate, over_cols, preferred_element_type=jnp.float32)
    slot_terms = slot_terms + lax.dot_general(
        up_back, w_up, over_cols, preferred_element_type=jnp.float32
    )
    gate_grad = lax.dot_general(
        token_rows, gate_back, over_rows, preferred_element_type=jnp.float32
    ).astype(jnp.bfloat16)[None]
    up_grad = lax.dot_general(
        token_rows, up_back, over_rows, preferred_element_type=jnp.float32
    ).astype(jnp.bfloat16)[None]
    down_grad = lax.dot_general(
        hidden, out_scaled, over_rows, preferred_element_type=jnp.float32
    ).astype(jnp.bfloat16)[None]
    back_rows, back_mix = combine(
        slot_terms.astype(jnp.bfloat16).reshape(senders, capacity, model_width),
        pad_lanes(mix_part.reshape(senders, capacity)),
    )
    back_flat = back_rows.reshape(experts * capacity, col_width)
    over_slots = (((0,), (0,)), ((), ()))
    token_part = lax.dot_general(pick, back_flat, over_slots, preferred_element_type=jnp.float32)
    mix_flat = back_mix[:, 0, :capacity].reshape(experts * capacity)
    mixing_grad = jnp.sum(jnp.where(hits, mix_flat[:, None, None], 0.0), axis=0).T
    pairwise = mixing[:, 0] * mixing[:, 1]
    logit_grad = pairwise[:, None] * (mixing_grad - mixing_grad[:, ::-1])
    route_grad = jnp.sum(jnp.where(picked, logit_grad[:, :, None], 0.0), axis=1)
    router_cols = lax.dynamic_slice_in_dim(
        router_matrix, tp_index * col_width, col_width, 0
    ).astype(jnp.float32)
    router_path = jnp.dot(route_grad, router_cols.T, precision=lax.Precision.HIGHEST)
    token_grad = (token_part + router_path).astype(jnp.bfloat16)
    row_share = model_width // (ep_size * tp_size)
    feature_share = lax.dynamic_slice_in_dim(
        tokens.reshape(home_rows, ep_size, tp_size, row_share), tp_index, 1, 2
    )
    feature_share = feature_share.reshape(home_rows, ep_size * row_share).astype(jnp.float32)
    norm_scale = 1.0 / math.sqrt(home_rows * ep_size)
    router_terms = (
        jnp.dot(route_grad.T, feature_share, precision=lax.Precision.HIGHEST) * norm_scale
    )
    router_terms = jnp.swapaxes(router_terms.reshape(experts, ep_size, row_share), 0, 1)
    router_terms = jnp.pad(router_terms, ((0, 0), (0, 0), (0, LANES - row_share)))
    router_grad = router_sum(router_terms)[:, :row_share].T
    return (token_grad, mixing_grad, router_grad, gate_grad, up_grad, down_grad)


def solution(mesh):
    return jax.shard_map(
        local,
        mesh=mesh,
        in_specs=(
            P("ep", None),
            P("ep", None),
            P(),
            P("ep", "tp"),
            P("ep", None, "tp"),
            P("ep", None, "tp"),
            P("ep", "tp", None),
        ),
        out_specs=(
            P("ep", "tp"),
            P("ep", None),
            P(("ep", "tp"), None),
            P("ep", None, "tp"),
            P("ep", None, "tp"),
            P("ep", "tp", None),
        ),
        check_vma=False,
    )
```
